32 devices in a mesh: rep: 1, fs: 8 (over z, y), tp: 4 (over x, core).
Axes of the slice: x: 2, y: 2, z: 4, core: 2. Of those that a mesh axis runs over, the one named last changes fastest.
Arguments:
- tokens: bfloat16 [4096, 2048], P(('rep', 'fs')), may hold values from -6 to 6
- gate_outer: bfloat16 [2048, 1024], P('fs', 'tp'), may hold values from -0.125 to 0.125
- gate_inner: bfloat16 [2048, 1024], P('fs', 'tp'), may hold values from -0.125 to 0.125
- conv_input: bfloat16 [2048, 1024], P('fs', 'tp'), may hold values from -0.125 to 0.125
- mixer_output: bfloat16 [2048, 1024], P('fs', 'tp'), may hold values from -0.1875 to 0.1875
- conv_taps: float32 [3, 1024], P(None, 'tp'), may hold values from -3 to 3
- mixer_gain: float32 [2048], replicated, may hold values from 0.1 to 1.9
- mixer_shift: float32 [2048], replicated, may hold values from -3 to 3
- up_weight: bfloat16 [2048, 8192], P('fs', 'tp'), may hold values from -0.125 to 0.125
- down_weight: bfloat16 [2048, 8192], P('fs', 'tp'), may hold values from -0.0625 to 0.0625
- channel_gain: float32 [2048], replicated, may hold values from 0.1 to 1.9
- channel_shift: float32 [2048], replicated, may hold values from -3 to 3
Outputs:
- mixed: bfloat16 [4096, 2048], P(('rep', 'fs'))
The draws below stay inside these ranges and needn't reach their ends.
All inputs are finite; a program needn't handle non-finite values.
Results may differ from the reference program's by a relative error of at most 0.014.
Values may be sent and summed in bfloat16 or wider, within the bound.
A program may use at most 64 MiB of HBM per device.

```python
import jax
import jax.numpy as jnp
from jax import lax

D = 2048
C = 1024
FF = 8192
TAPS = 3
LEN = 512
SEQS = 8
TOKENS = 4096
N_TP = 4


def levels(rng, dims, shards, least, top_value):
    loudness = 1.0
    for axis_at, parts in shards:
        steps = jax.random.uniform(jax.random.fold_in(jax.random.fold_in(rng, 6), axis_at), (parts,), jnp.float32, least / len(shards), top_value / len(shards))
        loudness = loudness * jnp.repeat(jnp.exp(steps), dims[axis_at] // parts).reshape((-1,) + (1,) * (len(dims) - 1 - axis_at))
    return loudness


def bell_draw(own_key, dims, deviation, most, pieces=(), dtype=jnp.bfloat16):
    drawn = jax.random.normal(own_key, dims, jnp.float32) * deviation
    if len(pieces) > 0:
        drawn = levels(own_key, dims, pieces, -0.22, 0.18) * drawn
    return jnp.clip(drawn, min=-most, max=most).astype(dtype)


def setup_inputs(seed: int = 0) -> dict:
    arg_keys = jax.random.split(jax.random.key(seed), 13)
    return {
        "tokens": bell_draw(arg_keys[0], (TOKENS, D), 1.0, 6.0, ((0, 8),)),
        "gate_outer": bell_draw(arg_keys[1], (D, C), D ** -0.5, 0.125, ((0, 8), (1, 4))),
        "gate_inner": bell_draw(arg_keys[2], (D, C), D ** -0.5, 0.125, ((0, 8), (1, 4))),
        "conv_input": bell_draw(arg_keys[3], (D, C), D ** -0.5, 0.125, ((0, 8), (1, 4))),
        "mixer_output": bell_draw(arg_keys[4], (D, C), C ** -0.5, 0.1875, ((0, 8), (1, 4))),
        "conv_taps": bell_draw(arg_keys[5], (TAPS, C), 0.6, 3.0, ((1, 4),), jnp.float32),
        "mixer_gain": jnp.clip(1.0 + 0.18 * jax.random.normal(arg_keys[6], (D,), jnp.float32), 0.1, 1.9),
        "mixer_shift": bell_draw(arg_keys[7], (D,), 0.5, 3.0, (), jnp.float32),
        "up_weight": bell_draw(arg_keys[8], (D, FF), D ** -0.5, 0.125, ((0, 8), (1, 4))),
        "down_weight": bell_draw(arg_keys[9], (D, FF), FF ** -0.5, 0.0625, ((0, 8), (1, 4))),
        "channel_gain": jnp.clip(1.0 + 0.18 * jax.random.normal(arg_keys[10], (D,), jnp.float32), 0.1, 1.9),
        "channel_shift": bell_draw(arg_keys[11], (D,), 0.5, 3.0, (), jnp.float32),
    }


residual_scale = 8.0 ** 0.25
norm_epsilon = 1e-05

def layer_norm(values, gain, shift):
    row_mean = lax.optimization_barrier(jnp.mean(values, -1, keepdims=True))
    centered = values - row_mean
    variance = lax.optimization_barrier(jnp.mean(centered * centered, -1, keepdims=True))
    return centered * lax.rsqrt(variance + norm_epsilon) * gain + shift

def blockwise_sum(left, right_t):
    block_width = left.shape[1] // N_TP
    totals = jnp.zeros((left.shape[0], right_t.shape[0]), jnp.float32)
    for block_index in range(N_TP):
        lower = block_index * block_width
        product = lax.dot_general(left[:, lower:lower + block_width], right_t[:, lower:lower + block_width], (((1,), (1,)), ((), ())), preferred_element_type=jnp.float32)
        totals = totals + lax.optimization_barrier(product.astype(jnp.bfloat16)).astype(jnp.float32)
    return totals

def reference(tokens, gate_outer, gate_inner, conv_input, mixer_output, conv_taps, mixer_gain, mixer_shift, up_weight, down_weight, channel_gain, channel_shift):

    def one_sequence(seq_rows):
        outer_gate = jnp.dot(seq_rows, gate_outer, preferred_element_type=jnp.float32)
        inner_gate = jnp.dot(seq_rows, gate_inner, preferred_element_type=jnp.float32)
        conv_values = jnp.dot(seq_rows, conv_input, preferred_element_type=jnp.float32)
        product = inner_gate * conv_values
        padded = jnp.pad(product, ((TAPS - 1, 0), (0, 0)))
        result = jnp.zeros_like(product)
        for tap_index in range(TAPS):
            result = result + conv_taps[tap_index] * padded[tap_index:tap_index + LEN]
        conv_out = (outer_gate * result).astype(jnp.bfloat16)
        mixer_sum = blockwise_sum(conv_out, mixer_output)
        first = layer_norm(residual_scale * seq_rows.astype(jnp.float32) + mixer_sum, mixer_gain, mixer_shift).astype(jnp.bfloat16)
        up_product = jnp.dot(first, up_weight, preferred_element_type=jnp.float32)
        hidden = jnp.square(jax.nn.relu(up_product)).astype(jnp.bfloat16)
        channel_sum = blockwise_sum(hidden, down_weight)
        return layer_norm(residual_scale * first.astype(jnp.float32) + channel_sum, channel_gain, channel_shift).astype(jnp.bfloat16)
    sequences = tokens.reshape(SEQS, LEN, D)
    outputs = lax.map(one_sequence, sequences)
    return outputs.reshape(TOKENS, D)
```

```python
import functools

import jax
import jax.numpy as jnp
from jax import lax
from jax.experimental import pallas as pl
from jax.experimental.pallas import tpu as pltpu
from jax.sharding import PartitionSpec as P

residual_scale = 8.0**0.25
norm_epsilon = 1e-05
MESH = pl.DeviceIdType.MESH
f32 = jnp.float32
bf16 = jnp.bfloat16
NT = (((1,), (1,)), ((), ()))


def layer_norm(values, gain, shift):
    row_mean = jnp.mean(values, -1, keepdims=True)
    centered = values - row_mean
    variance = jnp.mean(centered * centered, -1, keepdims=True)
    return centered * lax.rsqrt(variance + norm_epsilon) * gain + shift


def kernel(
    n_fs,
    n_tp,
    via,
    tokens,
    w_go,
    w_gi,
    w_ci,
    w_mo,
    taps,
    m_gain,
    m_shift,
    w_up,
    w_dn,
    c_gain,
    c_shift,
    out,
    mix_g,
    up_g,
    dn_g,
    outer,
    zpad,
    conv,
    part,
    part2,
    first,
    hidden,
    result,
    recv1,
    recv2,
    local_sem,
    gs_send,
    gs_recv,
    ts_send,
    ts_recv,
):
    seq, width = tokens.shape
    rows = w_up.shape[0]
    units = w_up.shape[1]
    bits = n_tp.bit_length() - 1
    nk = n_fs // 2
    f = lax.axis_index("fs")
    t = lax.axis_index("tp")
    k = f // 2
    p = f % 2
    partner = f + 1 - 2 * p
    has_right = k < nk - 1
    has_left = k > 0

    def flip(bit):
        return t + bit - 2 * bit * ((t // bit) % 2)

    own = pl.ds(pl.multiple_of(f * rows, rows), rows)
    copies = []
    for j, ref in enumerate((w_go, w_gi, w_ci, w_mo)):
        copies.append(pltpu.make_async_copy(ref, mix_g.at[j, own], local_sem.at[j]))
    copies.append(pltpu.make_async_copy(w_up, up_g.at[own], local_sem.at[4]))
    copies.append(pltpu.make_async_copy(w_dn, dn_g.at[own], local_sem.at[5]))
    for c in copies:
        c.start()

    barrier = pltpu.get_barrier_semaphore()
    pl.semaphore_signal(barrier, inc=1, device_id={"fs": partner}, device_id_type=MESH)

    @pl.when(has_right)
    def _():
        pl.semaphore_signal(barrier, inc=1, device_id={"fs": f + 2}, device_id_type=MESH)

    @pl.when(has_left)
    def _():
        pl.semaphore_signal(barrier, inc=1, device_id={"fs": f - 2}, device_id_type=MESH)

    for b in range(bits):
        pl.semaphore_signal(barrier, inc=1, device_id={"tp": flip(1 << b)}, device_id_type=MESH)
    neighbours = (k + nk - 1) // nk + (2 * nk - 2 - k) // nk
    pl.semaphore_wait(barrier, 1 + bits + neighbours)

    for c in copies:
        c.wait()

    bufs = (mix_g, up_g, dn_g)
    spans = ((0, rows - via), (rows - via, via))

    def piece(a, s, q):
        lo, n = spans[q]
        at = pl.ds(pl.multiple_of(s * rows + lo, 16), n)
        return bufs[a].at[:, at] if a == 0 else bufs[a].at[at]

    def copy(a, s, q, way):
        target = (partner, f + 2, f - 2)[way]
        ref = piece(a, s, q)
        return pltpu.make_async_remote_copy(
            src_ref=ref,
            dst_ref=ref,
            send_sem=gs_send.at[a, s, q, way],
            recv_sem=gs_recv.at[a, s, q],
            device_id={"fs": target},
            device_id_type=MESH,
        )

    def send(a, s, q, way):
        if way == 0:
            copy(a, s, q, 0).start()
        else:

            @pl.when(has_right if way == 1 else has_left)
            def _():
                copy(a, s, q, way).start()

    def arrive(a, s, q):
        copy(a, s, q, 0).wait_recv()

    def begin(a):
        for q in (0, 1):
            for way in (0, 1, 2):
                send(a, f, q, way)

    def after_pair(a):
        arrive(a, partner, 0)
        send(a, partner, 0, 1)
        send(a, partner, 0, 2)

    def step(a, d):
        for way, s, ok in ((1, f - 2 * d, k - d >= 0), (2, f + 2 * d, k + d < nk)):

            @pl.when(ok)
            def _(way=way, s=s):
                other = s + 1 - 2 * p
                for q in (1, 0):
                    arrive(a, s, q)
                    if q == 1:
                        send(a, s, q, 0)
                    send(a, s, q, way)
                arrive(a, other, 0)
                send(a, other, 0, way)

    def finish(a):
        arrive(a, partner, 1)
        for d in range(1, nk):
            for s, ok in ((f - 2 * d, k - d >= 0), (f + 2 * d, k + d < nk)):

                @pl.when(ok)
                def _(s=s):
                    arrive(a, s + 1 - 2 * p, 1)

    def drain(a):
        for q in (0, 1):
            copy(a, f, q, 0).wait_send()
            for way, has in ((1, has_right), (2, has_left)):

                @pl.when(has)
                def _(q=q, way=way):
                    copy(a, f, q, way).wait_send()
                    if q == 0:
                        copy(a, partner, q, way).wait_send()

        for d in range(1, nk):
            for way, s, ok in ((1, f - 2 * d, k - d >= 0), (2, f + 2 * d, k + d < nk)):

                @pl.when(ok)
                def _(way=way, s=s):
                    copy(a, s, 1, 0).wait_send()

                    @pl.when(has_right if way == 1 else has_left)
                    def _():
                        copy(a, s, 0, way).wait_send()
                        copy(a, s, 1, way).wait_send()
                        copy(a, s + 1 - 2 * p, 0, way).wait_send()

    starts = [0]
    for b in range(bits):
        starts.append(starts[-1] + ((t // (1 << b)) % 2) * (seq >> (b + 1)))

    def block_rows(start, b):
        return pl.ds(pl.multiple_of(start, seq >> b), seq >> b)

    def tp_copy(kind, src, dst, b):
        return pltpu.make_async_remote_copy(
            src_ref=src,
            dst_ref=dst,
            send_sem=ts_send.at[kind, b],
            recv_sem=ts_recv.at[kind, b],
            device_id={"tp": flip(1 << b)},
            device_id_type=MESH,
        )

    def reduce_copy(kind, source, landing, b):
        n = seq >> (b + 1)
        away = starts[b] + (1 - (t // (1 << b)) % 2) * n
        base = seq - (seq >> b)
        return tp_copy(kind, source.at[block_rows(away, b + 1)], landing.at[pl.ds(base, n)], b)

    def reduce_add(source, landing, b):
        n = seq >> (b + 1)
        base = seq - (seq >> b)
        tile = min(n, 32)

        @pl.loop(0, n // tile)
        def _(i):
            mine = pl.ds(pl.multiple_of(starts[b + 1] + i * tile, tile), tile)
            theirs = pl.ds(pl.multiple_of(base + i * tile, tile), tile)
            source[mine] = (source[mine].astype(f32) + landing[theirs].astype(f32)).astype(bf16)

    def gather_copy(kind, buf, b):
        ref = buf.at[block_rows(starts[b + 1], b + 1)]
        return tp_copy(kind, ref, ref, b)

    def norm_own(residual, source, landing, gain, shift, dest):
        b = bits - 1
        n = seq >> bits
        base = seq - (seq >> b)
        tile = min(n, 16)

        @pl.loop(0, n // tile)
        def _(i):
            mine = pl.ds(pl.multiple_of(starts[bits] + i * tile, tile), tile)
            theirs = pl.ds(pl.multiple_of(base + i * tile, tile), tile)
            total = source[mine].astype(f32) + landing[theirs].astype(f32)
            dest[mine] = layer_norm(
                residual_scale * residual[mine].astype(f32) + total, gain[...], shift[...]
            ).astype(bf16)

    begin(0)
    after_pair(0)
    for d in range(1, nk):
        step(0, d)
    begin(1)
    finish(0)

    pad = zpad.shape[0] - seq
    zpad[0:pad] = jnp.zeros((pad, zpad.shape[1]), f32)
    tile = seq // 2

    @pl.loop(0, 2)
    def _(i):
        at = pl.ds(pl.multiple_of(i * tile, tile), tile)
        x = tokens[at]
        outer[at] = jnp.dot(x, mix_g[0], preferred_element_type=f32)
        inner = jnp.dot(x, mix_g[1], preferred_element_type=f32)
        values = jnp.dot(x, mix_g[2], preferred_element_type=f32)
        zpad[pl.ds(pl.multiple_of(i * tile + pad, 8), tile)] = inner * values

    n_taps = taps.shape[0]
    acc = jnp.zeros((seq, zpad.shape[1]), f32)
    for j in range(n_taps):
        lo = pad - (n_taps - 1) + j
        acc = acc + taps[j : j + 1] * zpad[lo : lo + seq]
    conv[...] = (outer[...] * acc).astype(bf16)
    wide = min(256, width)

    @pl.loop(0, width // wide)
    def _(i):
        at = pl.ds(pl.multiple_of(i * wide, wide), wide)
        part[:, at] = lax.dot_general(
            conv[...], mix_g[3, at], NT, preferred_element_type=f32
        ).astype(bf16)

    stages = []
    for b in range(bits):
        c = reduce_copy(0, part, recv1, b)
        stages.append(c.start)
        if b < bits - 1:
            stages.append(lambda c=c, b=b: (c.wait_recv(), reduce_add(part, recv1, b)))
        else:
            stages.append(
                lambda c=c: (
                    c.wait_recv(),
                    norm_own(tokens, part, recv1, m_gain, m_shift, first),
                )
            )
    for b in reversed(range(bits)):
        c = gather_copy(1, first, b)
        stages.append(c.start)
        stages.append(c.wait_recv)
    groups = [stages[:1]]
    for i in range(1, len(stages) - 1, 2):
        groups.append(stages[i : i + 2])
    groups.append(stages[-1:])

    def run(group):
        for g in group:
            g()

    run(groups.pop(0))
    after_pair(1)
    for d in range(1, nk):
        if groups:
            run(groups.pop(0))
        step(1, d)
    begin(2)
    while groups:
        run(groups.pop(0))
    finish(1)
    after_pair(2)

    wide_u = min(256, units)

    @pl.loop(0, units // wide_u)
    def _(i):
        at = pl.ds(pl.multiple_of(i * wide_u, wide_u), wide_u)
        u = jnp.maximum(jnp.dot(first[...], up_g[:, at], preferred_element_type=f32), 0.0)
        hidden[:, at] = (u * u).astype(bf16)

    for d in range(1, nk):
        step(2, d)
    finish(2)

    @pl.loop(0, width // wide)
    def _(i):
        at = pl.ds(pl.multiple_of(i * wide, wide), wide)
        part2[:, at] = lax.dot_general(
            hidden[...], dn_g[at], NT, preferred_element_type=f32
        ).astype(bf16)

    for b in range(bits):
        c = reduce_copy(2, part2, recv2, b)
        c.start()
        c.wait_recv()
        if b < bits - 1:
            reduce_add(part2, recv2, b)
        else:
            norm_own(first, part2, recv2, c_gain, c_shift, result)
    for b in reversed(range(bits)):
        c = gather_copy(3, result, b)
        c.start()
        c.wait_recv()
    done = pltpu.make_async_copy(result, out, local_sem.at[6])
    done.start()

    for a in range(3):
        drain(a)
    for b in range(bits):
        reduce_copy(0, part, recv1, b).wait_send()
        gather_copy(1, first, b).wait_send()
        reduce_copy(2, part2, recv2, b).wait_send()
        gather_copy(3, result, b).wait_send()
    done.wait()


def local(
    tokens,
    gate_outer,
    gate_inner,
    conv_input,
    mixer_output,
    conv_taps,
    mixer_gain,
    mixer_shift,
    up_weight,
    down_weight,
    channel_gain,
    channel_shift,
):
    seq, width = tokens.shape
    rows, units = up_weight.shape
    chans = gate_outer.shape[1]
    n_fs = lax.axis_size("fs")
    n_tp = lax.axis_size("tp")
    bits = n_tp.bit_length() - 1
    via = max(16, rows * 13 // 16 // 16 * 16)
    vmem = pl.BlockSpec(memory_space=pltpu.VMEM)
    return pl.pallas_call(
        functools.partial(kernel, n_fs, n_tp, via),
        out_shape=jax.ShapeDtypeStruct((seq, width), bf16),
        in_specs=[vmem] * 12,
        out_specs=pl.BlockSpec(memory_space=pl.ANY),
        scratch_shapes=[
            pltpu.VMEM((4, width, chans), bf16),
            pltpu.VMEM((width, units), bf16),
            pltpu.VMEM((width, units), bf16),
            pltpu.VMEM((seq, chans), f32),
            pltpu.VMEM((seq + 8, chans), f32),
            pltpu.VMEM((seq, chans), bf16),
            pltpu.VMEM((seq, width), bf16),
            pltpu.VMEM((seq, width), bf16),
            pltpu.VMEM((seq, width), bf16),
            pltpu.VMEM((seq, units), bf16),
            pltpu.VMEM((seq, width), bf16),
            pltpu.VMEM((seq, width), bf16),
            pltpu.VMEM((seq, width), bf16),
            pltpu.SemaphoreType.DMA((7,)),
            pltpu.SemaphoreType.DMA((3, n_fs, 2, 3)),
            pltpu.SemaphoreType.DMA((3, n_fs, 2)),
            pltpu.SemaphoreType.DMA((4, bits)),
            pltpu.SemaphoreType.DMA((4, bits)),
        ],
        compiler_params=pltpu.CompilerParams(
            collective_id=0, has_side_effects=True, vmem_limit_bytes=62 * 1024 * 1024
        ),
    )(
        tokens,
        gate_outer,
        gate_inner,
        conv_input,
        mixer_output,
        conv_taps,
        mixer_gain.reshape(1, width),
        mixer_shift.reshape(1, width),
        up_weight,
        down_weight,
        channel_gain.reshape(1, width),
        channel_shift.reshape(1, width),
    )


def solution(mesh):
    in_specs = (
        P(("rep", "fs"), None),
        P("fs", "tp"),
        P("fs", "tp"),
        P("fs", "tp"),
        P("fs", "tp"),
        P(None, "tp"),
        P(),
        P(),
        P("fs", "tp"),
        P("fs", "tp"),
        P(),
        P(),
    )
    out_specs = P(("rep", "fs"), None)
    return jax.shard_map(local, mesh=mesh, in_specs=in_specs, out_specs=out_specs, check_vma=False)
```

```python
import functools

import jax
import jax.numpy as jnp
from jax import lax
from jax.experimental import pallas as pl
from jax.experimental.pallas import tpu as pltpu
from jax.sharding import PartitionSpec as P

residual_scale = 8.0**0.25
norm_epsilon = 1e-05
MESH = pl.DeviceIdType.MESH
f32 = jnp.float32
bf16 = jnp.bfloat16
NT = (((1,), (1,)), ((), ()))


def layer_norm(values, gain, shift):
    row_mean = jnp.mean(values, -1, keepdims=True)
    centered = values - row_mean
    variance = jnp.mean(centered * centered, -1, keepdims=True)
    return centered * lax.rsqrt(variance + norm_epsilon) * gain + shift


def kernel(
    n_fs,
    n_tp,
    via,
    tokens,
    w_go,
    w_gi,
    w_ci,
    w_mo,
    taps,
    m_gain,
    m_shift,
    w_up,
    w_dn,
    c_gain,
    c_shift,
    out,
    mix_g,
    up_g,
    dn_g,
    outer,
    zpad,
    conv,
    part,
    part2,
    first,
    hidden,
    result,
    recv1,
    recv2,
    local_sem,
    gs_send,
    gs_recv,
    ts_send,
    ts_recv,
    ms_send,
    ms_recv,
    ps_send,
    ps_recv,
):
    seq, width = tokens.shape
    rows = w_up.shape[0]
    units = w_up.shape[1]
    bits = n_tp.bit_length() - 1
    nk = n_fs // 2
    f = lax.axis_index("fs")
    t = lax.axis_index("tp")
    k = f // 2
    p = f % 2
    partner = f + 1 - 2 * p
    e = k % 2
    mate = f + 2 - 4 * e
    half = units // 2
    mine_off = e * seq
    mate_off = (1 - e) * seq
    has_right = k < nk - 1
    has_left = k > 0
    has_right2 = k < nk - 2
    has_left2 = k > 1

    def flip(bit):
        return t + bit - 2 * bit * ((t // bit) % 2)

    own = pl.ds(pl.multiple_of(f * rows, rows), rows)
    copies = []
    for j, ref in enumerate((w_go, w_gi, w_ci, w_mo)):
        copies.append(pltpu.make_async_copy(ref, mix_g.at[j, own], local_sem.at[j]))
    keep_cols = pl.ds(pl.multiple_of(e * half, half), half)
    away_cols = pl.ds(pl.multiple_of((1 - e) * half, half), half)
    for j, (w, g) in enumerate(((w_up, up_g), (w_dn, dn_g))):
        copies.append(pltpu.make_async_copy(w.at[:, keep_cols], g.at[own], local_sem.at[4 + j]))
    for c in copies:
        c.start()

    barrier = pltpu.get_barrier_semaphore()
    pl.semaphore_signal(barrier, inc=1, device_id={"fs": partner}, device_id_type=MESH)

    @pl.when(has_right)
    def _():
        pl.semaphore_signal(barrier, inc=1, device_id={"fs": f + 2}, device_id_type=MESH)

    @pl.when(has_left)
    def _():
        pl.semaphore_signal(barrier, inc=1, device_id={"fs": f - 2}, device_id_type=MESH)

    @pl.when(has_right2)
    def _():
        pl.semaphore_signal(barrier, inc=1, device_id={"fs": f + 4}, device_id_type=MESH)

    @pl.when(has_left2)
    def _():
        pl.semaphore_signal(barrier, inc=1, device_id={"fs": f - 4}, device_id_type=MESH)

    for b in range(bits):
        pl.semaphore_signal(barrier, inc=1, device_id={"tp": flip(1 << b)}, device_id_type=MESH)
    neighbours = (k + nk - 1) // nk + (2 * nk - 2 - k) // nk
    neighbours += (k + nk - 2) // nk + (2 * nk - 3 - k) // nk
    pl.semaphore_wait(barrier, 1 + bits + neighbours)

    for c in copies:
        c.wait()

    spans = ((0, rows - via), (rows - via, via))

    def piece(a, s, q):
        lo, n = spans[q]
        at = pl.ds(pl.multiple_of(s * rows + lo, 16), n)
        return mix_g.at[:, at]

    def copy(a, s, q, way):
        target = (partner, f + 2, f - 2)[way]
        ref = piece(a, s, q)
        return pltpu.make_async_remote_copy(
            src_ref=ref,
            dst_ref=ref,
            send_sem=gs_send.at[a, s, q, way],
            recv_sem=gs_recv.at[a, s, q],
            device_id={"fs": target},
            device_id_type=MESH,
        )

    def send(a, s, q, way):
        if way == 0:
            copy(a, s, q, 0).start()
        else:

            @pl.when(has_right if way == 1 else has_left)
            def _():
                copy(a, s, q, way).start()

    def arrive(a, s, q):
        copy(a, s, q, 0).wait_recv()

    def begin(a):
        for q in (0, 1):
            for way in (0, 1, 2):
                send(a, f, q, way)

    def after_pair(a):
        arrive(a, partner, 0)
        send(a, partner, 0, 1)
        send(a, partner, 0, 2)

    def step(a, d):
        for way, s, ok in ((1, f - 2 * d, k - d >= 0), (2, f + 2 * d, k + d < nk)):

            @pl.when(ok)
            def _(way=way, s=s):
                other = s + 1 - 2 * p
                for q in (1, 0):
                    arrive(a, s, q)
                    if q == 1:
                        send(a, s, q, 0)
                    send(a, s, q, way)
                arrive(a, other, 0)
                send(a, other, 0, way)

    def finish(a):
        arrive(a, partner, 1)
        for d in range(1, nk):
            for s, ok in ((f - 2 * d, k - d >= 0), (f + 2 * d, k + d < nk)):

                @pl.when(ok)
                def _(s=s):
                    arrive(a, s + 1 - 2 * p, 1)

    def drain(a):
        for q in (0, 1):
            copy(a, f, q, 0).wait_send()
            for way, has in ((1, has_right), (2, has_left)):

                @pl.when(has)
                def _(q=q, way=way):
                    copy(a, f, q, way).wait_send()
                    if q == 0:
                        copy(a, partner, q, way).wait_send()

        for d in range(1, nk):
            for way, s, ok in ((1, f - 2 * d, k - d >= 0), (2, f + 2 * d, k + d < nk)):

                @pl.when(ok)
                def _(way=way, s=s):
                    copy(a, s, 1, 0).wait_send()

                    @pl.when(has_right if way == 1 else has_left)
                    def _():
                        copy(a, s, 0, way).wait_send()
                        copy(a, s, 1, way).wait_send()
                        copy(a, s + 1 - 2 * p, 0, way).wait_send()

    def half_copy(a, s, way):
        w, g = ((w_up, up_g), (w_dn, dn_g))[a]
        dst = g.at[pl.ds(pl.multiple_of(s * rows, rows), rows)]
        src = w.at[:, away_cols] if way > 2 else dst
        return pltpu.make_async_remote_copy(
            src_ref=src,
            dst_ref=dst,
            send_sem=ms_send.at[a, s, way],
            recv_sem=ms_recv.at[a, s],
            device_id={"fs": (partner, f + 4, f - 4, f + 2, f - 2)[way]},
            device_id_type=MESH,
        )

    exists = (None, has_right2, has_left2, has_right, has_left)

    def half_each(a, s, ways, act):
        for way in ways:
            if way == 0:
                act(half_copy(a, s, way))
            else:

                @pl.when(exists[way])
                def _(way=way):
                    act(half_copy(a, s, way))

    def half_begin(a):
        half_each(a, f, (3, 4, 1, 2, 0), lambda c: c.start())

    def half_sides(d):
        return ((1, f - 2 * d, k - d >= 0), (2, f + 2 * d, k + d < nk))

    def half_step(a, d):
        for way, s, ok in half_sides(d):

            @pl.when(ok)
            def _(way=way, s=s):
                half_copy(a, s, 0).wait_recv()
                half_each(a, s, (way, 0), lambda c: c.start())

    def half_finish(a):
        half_copy(a, partner, 0).wait_recv()
        for d in range(1, nk):
            for way, s, ok in half_sides(d):

                @pl.when(ok)
                def _(s=s):
                    half_copy(a, s + 1 - 2 * p, 0).wait_recv()

    def half_drain(a):
        half_each(a, f, (0, 1, 2, 3, 4), lambda c: c.wait_send())
        for d in range(1, nk):
            for way, s, ok in half_sides(d):

                @pl.when(ok)
                def _(way=way, s=s):
                    half_each(a, s, (way, 0), lambda c: c.wait_send())

    starts = [0]
    for b in range(bits):
        starts.append(starts[-1] + ((t // (1 << b)) % 2) * (seq >> (b + 1)))

    def block_rows(start, b, off=0):
        return pl.ds(pl.multiple_of(off + start, seq >> b), seq >> b)

    def tp_copy(kind, src, dst, b):
        return pltpu.make_async_remote_copy(
            src_ref=src,
            dst_ref=dst,
            send_sem=ts_send.at[kind, b],
            recv_sem=ts_recv.at[kind, b],
            device_id={"tp": flip(1 << b)},
            device_id_type=MESH,
        )

    def reduce_copy(kind, source, landing, b, off=0, land=0):
        n = seq >> (b + 1)
        away = starts[b] + (1 - (t // (1 << b)) % 2) * n
        base = land + seq - (seq >> b)
        return tp_copy(
            kind, source.at[block_rows(away, b + 1, off)], landing.at[pl.ds(base, n)], b
        )

    def add_rows(source, start, landing, base, n):
        tile = min(n, 16)

        @pl.loop(0, n // tile)
        def _(i):
            mine = pl.ds(pl.multiple_of(start + i * tile, tile), tile)
            theirs = pl.ds(pl.multiple_of(base + i * tile, tile), tile)
            source[mine] = (source[mine].astype(f32) + landing[theirs].astype(f32)).astype(bf16)

    def reduce_add(source, landing, b, off=0, land=0):
        add_rows(source, off + starts[b + 1], landing, land + seq - (seq >> b), seq >> (b + 1))

    def gather_copy(kind, buf, b, off=0):
        ref = buf.at[block_rows(starts[b + 1], b + 1, off)]
        return tp_copy(kind, ref, ref, b)

    def pair_copy(i, src, dst, to_mate):
        return pltpu.make_async_remote_copy(
            src_ref=src,
            dst_ref=dst,
            send_sem=ps_send.at[i],
            recv_sem=ps_recv.at[i],
            device_id={"fs": mate} if to_mate else {"tp": flip(1)},
            device_id_type=MESH,
        )

    def norm_own(residual, source, landing, gain, shift, dest, off_r, off_s, land, off_d):
        n = seq >> bits
        base = land + seq - (seq >> (bits - 1))
        tile = min(n, 16)

        @pl.loop(0, n // tile)
        def _(i):
            at = starts[bits] + i * tile

            def rows_at(off):
                return pl.ds(pl.multiple_of(off + at, tile), tile)

            theirs = pl.ds(pl.multiple_of(base + i * tile, tile), tile)
            total = source[rows_at(off_s)].astype(f32) + landing[theirs].astype(f32)
            dest[rows_at(off_d)] = layer_norm(
                residual_scale * residual[rows_at(off_r)].astype(f32) + total,
                gain[...],
                shift[...],
            ).astype(bf16)

    begin(0)
    after_pair(0)
    for d in range(1, nk):
        step(0, d)
    half_begin(0)
    finish(0)

    pad = zpad.shape[0] - seq
    zpad[0:pad] = jnp.zeros((pad, zpad.shape[1]), f32)
    tile = seq // 2

    @pl.loop(0, 2)
    def _(i):
        at = pl.ds(pl.multiple_of(i * tile, tile), tile)
        x = tokens[at]
        outer[at] = jnp.dot(x, mix_g[0], preferred_element_type=f32)
        inner = jnp.dot(x, mix_g[1], preferred_element_type=f32)
        values = jnp.dot(x, mix_g[2], preferred_element_type=f32)
        zpad[pl.ds(pl.multiple_of(i * tile + pad, 8), tile)] = inner * values

    n_taps = taps.shape[0]
    acc = jnp.zeros((seq, zpad.shape[1]), f32)
    for j in range(n_taps):
        lo = pad - (n_taps - 1) + j
        acc = acc + taps[j : j + 1] * zpad[lo : lo + seq]
    conv[...] = (outer[...] * acc).astype(bf16)
    wide = min(256, width)

    @pl.loop(0, width // wide)
    def _(i):
        at = pl.ds(pl.multiple_of(i * wide, wide), wide)
        part[:, at] = lax.dot_general(
            conv[...], mix_g[3, at], NT, preferred_element_type=f32
        ).astype(bf16)

    stages = []
    for b in range(bits):
        c = reduce_copy(0, part, recv1, b)
        stages.append(c.start)
        if b < bits - 1:
            stages.append(lambda c=c, b=b: (c.wait_recv(), reduce_add(part, recv1, b)))
        else:
            stages.append(
                lambda c=c: (
                    c.wait_recv(),
                    norm_own(tokens, part, recv1, m_gain, m_shift, first, 0, 0, 0, mine_off),
                )
            )
    n0 = seq // 2
    for b in reversed(range(1, bits)):
        c = gather_copy(1, first, b, mine_off)
        stages.append(c.start)
        stages.append(c.wait_recv)
    held = first.at[block_rows(starts[1], 1, mine_off)]
    to_mate = pair_copy(0, held, held, True)
    stages.append(to_mate.start)
    stages.append(to_mate.wait_recv)
    across = []
    for q in (0, 1):
        ref = first.at[block_rows(starts[1], 1, q * seq)]
        across.append(pair_copy(1 + q, ref, ref, False))
    stages.append(lambda: [c.start() for c in across])
    stages.append(lambda: [c.wait_recv() for c in across])
    groups = [stages[:1]]
    for i in range(1, len(stages) - 1, 2):
        groups.append(stages[i : i + 2])
    groups.append(stages[-1:])

    def run(group):
        for g in group:
            g()

    run(groups.pop(0))
    for d in range(1, nk):
        if groups:
            run(groups.pop(0))
        half_step(0, d)
    half_begin(1)
    half_step(1, 1)
    while groups:
        run(groups.pop(0))
    half_finish(0)

    wide_u = min(256, half)

    @pl.loop(0, half // wide_u)
    def _(i):
        at = pl.ds(pl.multiple_of(i * wide_u, wide_u), wide_u)
        u = jnp.maximum(jnp.dot(first[...], up_g[:, at], preferred_element_type=f32), 0.0)
        hidden[:, at] = (u * u).astype(bf16)

    for d in range(2, nk):
        half_step(1, d)
    half_finish(1)

    @pl.loop(0, width // wide)
    def _(i):
        at = pl.ds(pl.multiple_of(i * wide, wide), wide)
        part2[:, at] = lax.dot_general(
            hidden[...], dn_g[at], NT, preferred_element_type=f32
        ).astype(bf16)

    over = []
    for q in (0, 1):
        away = (1 - t % 2) * n0
        over.append(
            pair_copy(
                3 + q, part2.at[block_rows(away, 1, q * seq)], recv2.at[pl.ds(q * n0, n0)], False
            )
        )
    for c in over:
        c.start()
    for c in over:
        c.wait_recv()
    add_rows(part2, mate_off + starts[1], recv2, (1 - e) * n0, n0)
    swap = pair_copy(
        5, part2.at[block_rows(starts[1], 1, mate_off)], recv2.at[pl.ds(seq, n0)], True
    )
    swap.start()
    add_rows(part2, mine_off + starts[1], recv2, e * n0, n0)
    swap.wait_recv()
    add_rows(part2, mine_off + starts[1], recv2, seq, n0)
    for b in range(1, bits):
        c = reduce_copy(2, part2, recv2, b, mine_off, seq)
        c.start()
        c.wait_recv()
        if b < bits - 1:
            reduce_add(part2, recv2, b, mine_off, seq)
    norm_own(first, part2, recv2, c_gain, c_shift, result, mine_off, mine_off, seq, 0)
    for b in reversed(range(bits)):
        c = gather_copy(3, result, b)
        c.start()
        c.wait_recv()
    done = pltpu.make_async_copy(result, out, local_sem.at[6])
    done.start()

    drain(0)
    half_drain(0)
    half_drain(1)
    for b in range(bits):
        reduce_copy(0, part, recv1, b).wait_send()
        gather_copy(3, result, b).wait_send()
        if b > 0:
            gather_copy(1, first, b, mine_off).wait_send()
            reduce_copy(2, part2, recv2, b, mine_off, seq).wait_send()
    for c in [to_mate, swap] + across + over:
        c.wait_send()
    done.wait()


def local(
    tokens,
    gate_outer,
    gate_inner,
    conv_input,
    mixer_output,
    conv_taps,
    mixer_gain,
    mixer_shift,
    up_weight,
    down_weight,
    channel_gain,
    channel_shift,
):
    seq, width = tokens.shape
    rows, units = up_weight.shape
    chans = gate_outer.shape[1]
    n_fs = lax.axis_size("fs")
    n_tp = lax.axis_size("tp")
    bits = n_tp.bit_length() - 1
    via = max(16, rows * 13 // 16 // 16 * 16)
    vmem = pl.BlockSpec(memory_space=pltpu.VMEM)
    return pl.pallas_call(
        functools.partial(kernel, n_fs, n_tp, via),
        out_shape=jax.ShapeDtypeStruct((seq, width), bf16),
        in_specs=[vmem] * 12,
        out_specs=pl.BlockSpec(memory_space=pl.ANY),
        scratch_shapes=[
            pltpu.VMEM((4, width, chans), bf16),
            pltpu.VMEM((width, units // 2), bf16),
            pltpu.VMEM((width, units // 2), bf16),
            pltpu.VMEM((seq, chans), f32),
            pltpu.VMEM((seq + 8, chans), f32),
            pltpu.VMEM((seq, chans), bf16),
            pltpu.VMEM((seq, width), bf16),
            pltpu.VMEM((2 * seq, width), bf16),
            pltpu.VMEM((2 * seq, width), bf16),
            pltpu.VMEM((2 * seq, units // 2), bf16),
            pltpu.VMEM((seq, width), bf16),
            pltpu.VMEM((seq, width), bf16),
            pltpu.VMEM((2 * seq, width), bf16),
            pltpu.SemaphoreType.DMA((7,)),
            pltpu.SemaphoreType.DMA((1, n_fs, 2, 3)),
            pltpu.SemaphoreType.DMA((1, n_fs, 2)),
            pltpu.SemaphoreType.DMA((4, bits)),
            pltpu.SemaphoreType.DMA((4, bits)),
            pltpu.SemaphoreType.DMA((2, n_fs, 5)),
            pltpu.SemaphoreType.DMA((2, n_fs)),
            pltpu.SemaphoreType.DMA((6,)),
            pltpu.SemaphoreType.DMA((6,)),
        ],
        compiler_params=pltpu.CompilerParams(
            collective_id=0, has_side_effects=True, vmem_limit_bytes=62 * 1024 * 1024
        ),
    )(
        tokens,
        gate_outer,
        gate_inner,
        conv_input,
        mixer_output,
        conv_taps,
        mixer_gain.reshape(1, width),
        mixer_shift.reshape(1, width),
        up_weight,
        down_weight,
        channel_gain.reshape(1, width),
        channel_shift.reshape(1, width),
    )


def solution(mesh):
    in_specs = (
        P(("rep", "fs"), None),
        P("fs", "tp"),
        P("fs", "tp"),
        P("fs", "tp"),
        P("fs", "tp"),
        P(None, "tp"),
        P(),
        P(),
        P("fs", "tp"),
        P("fs", "tp"),
        P(),
        P(),
    )
    out_specs = P(("rep", "fs"), None)
    return jax.shard_map(local, mesh=mesh, in_specs=in_specs, out_specs=out_specs, check_vma=False)
```
